256 devices in a mesh: sp: 32 (over z, y), fs: 4 (over x), tp: 2 (over core).
Axes of the slice: x: 4, y: 4, z: 8, core: 2. Of those that a mesh axis runs over, the one named last changes fastest.
Arguments:
- tokens: bfloat16 [4, 8192, 2048], P('fs', ('sp', 'tp')), may hold values from -6 to 6
- norm_gain: float32 [2048], replicated, may hold values from 0.1 to 1.9
- w_conv_gate: bfloat16 [2048, 1024], P('sp', 'tp'), may hold values from -0.125 to 0.125
- w_conv_in: bfloat16 [2048, 1024], P('sp', 'tp'), may hold values from -0.125 to 0.125
- w_conv_value: bfloat16 [2048, 1024], P('sp', 'tp'), may hold values from -0.125 to 0.125
- conv_taps: float32 [3, 1024], P(None, 'tp'), may hold values from -3.5 to 3.5
- w_receptance: bfloat16 [2048, 1024], P('sp', 'tp'), may hold values from -0.125 to 0.125
- w_key: bfloat16 [2048, 1024], P('sp', 'tp'), may hold values from -0.125 to 0.125
- w_value: bfloat16 [2048, 1024], P('sp', 'tp'), may hold values from -0.125 to 0.125
- w_decay_down: bfloat16 [2048, 128], P('sp'), may hold values from -0.125 to 0.125
- w_decay_up: bfloat16 [128, 1024], P(None, 'tp'), may hold values from -0.75 to 0.75
- decay_base: float32 [1024], P('tp'), may hold values from -12.5 to -3
- decay_shift: float32 [4, 8192, 1024], P('fs', 'sp', 'tp'), may hold values from -2.1 to 0
- w_rate_down: bfloat16 [2048, 128], P('sp'), may hold values from -0.125 to 0.125
- w_rate_up: bfloat16 [128, 1024], P(None, 'tp'), may hold values from -0.5 to 0.5
- rate_base: float32 [1024], P('tp'), may hold values from -10 to 1
- key_scale: float32 [1024], P('tp'), may hold values from 0.25 to 2.5
- key_mix: float32 [1024], P('tp'), may hold values from 0.1 to 0.7
- group_gain: float32 [1024], P('tp'), may hold values from 0.1 to 1.9
- w_out_conv: bfloat16 [1024, 2048], P('tp', 'sp'), may hold values from -0.125 to 0.125
- w_out_state: bfloat16 [1024, 2048], P('tp', 'sp'), may hold values from -0.125 to 0.125
Outputs:
- mixed: bfloat16 [4, 8192, 2048], P('fs', ('sp', 'tp'))
The draws below stay inside these ranges and needn't reach their ends.
All inputs are finite; a program needn't handle non-finite values.
Results may differ from the reference program's by a relative error of at most 0.015.
Values may be sent and summed in bfloat16 or wider, within the bound.
No kernel may reach another device: no remote copies, remote signals or barrier semaphores. Data moves between devices by JAX's collectives and lax.ppermute only.
A program may use at most 128 MiB of HBM per device.

```python
import math
import jax
import jax.numpy as jnp
from jax import lax

D = 2048
CONV_CH = 1024
HEADS = 16
HEAD = 64
DECAY_RANK = 128
RATE_RANK = 128
TOK_DEV = 256
STATE_CH = 1024
SERIES_STEPS = 8192
BATCH_SERIES = 4
N_TP = 2


def quick_head_count(key):
    head_count = STATE_CH // HEAD
    order = jax.random.permutation(jax.random.fold_in(key, 101), head_count)
    chosen = order < head_count // 2
    return jnp.repeat(chosen, HEAD)


def draw_decay_base(key, part):
    jitter = jax.random.uniform(jax.random.fold_in(key, 202), (STATE_CH,), jnp.float32, -0.5, 0.5)
    return jnp.where(quick_head_count(key), -3.5 + jitter, -12.0 + jitter)


def draw_rate_base(key, part):
    quick = jax.random.uniform(jax.random.fold_in(key, 303), (STATE_CH,), jnp.float32, -1.0, 1.0)
    slower = jax.random.uniform(jax.random.fold_in(key, 404), (STATE_CH,), jnp.float32, -10.0, -8.0)
    return jnp.where(quick_head_count(key), quick, slower)


def draw_decay_shift(key, part):
    block_count = SERIES_STEPS // TOK_DEV
    levels = jnp.exp(jax.random.uniform(jax.random.fold_in(key, 505), (BATCH_SERIES, block_count, 1, 1), jnp.float32, math.log(3e-06), math.log(6e-05)))
    rough = jnp.exp(jax.random.uniform(jax.random.fold_in(key, 606), (BATCH_SERIES, block_count, TOK_DEV, STATE_CH), jnp.float32, math.log(0.5), math.log(2.0)))
    drift = -(levels * rough).reshape(BATCH_SERIES, SERIES_STEPS, STATE_CH)
    spike_location = jax.random.randint(jax.random.fold_in(key, 707), (BATCH_SERIES, 3), 0, SERIES_STEPS)
    losses = jnp.log(jax.random.uniform(jax.random.fold_in(key, 808), (BATCH_SERIES, 3, STATE_CH), jnp.float32, 0.5, 0.8))
    slot_numbers = jnp.arange(SERIES_STEPS)
    spike_total = (slot_numbers[None, None, :] == spike_location[:, :, None]).astype(jnp.float32)
    return drift + jnp.einsum('sbl,sbc->slc', spike_total, losses)


def level_of(key, dims, split, low, high):
    loudness, own = 1.0, jax.random.fold_in(key, 6)
    for dim, blocks in split:
        heights = jnp.exp(jax.random.uniform(jax.random.fold_in(own, dim), (blocks,), jnp.float32, low / len(split), high / len(split)))
        loudness = loudness * jnp.repeat(heights, dims[dim] // blocks).reshape([-1 if axis == dim else 1 for axis in range(len(dims))])
    return loudness


def scatter_about(rng, extent, width, bound, cuts=(), kind=jnp.bfloat16):
    factor_of = level_of(rng, extent, cuts, -0.22, 0.18) if cuts else 1.0
    entries = jax.random.normal(rng, extent, jnp.float32) * width * factor_of
    return jnp.minimum(jnp.maximum(entries, -bound), bound).astype(kind)


def setup_inputs(seed: int = 0) -> dict:
    streams_of = jax.random.split(jax.random.key(seed), 22)
    return {
        "tokens": scatter_about(streams_of[0], (BATCH_SERIES, SERIES_STEPS, D), 1.0, 6.0, ((0, 4), (1, 64))),
        "norm_gain": jnp.clip(1.0 + 0.18 * jax.random.normal(streams_of[1], (D,), jnp.float32), 0.1, 1.9),
        "w_conv_gate": scatter_about(streams_of[2], (D, CONV_CH), D ** -0.5, 0.125, ((0, 32), (1, 2))),
        "w_conv_in": scatter_about(streams_of[3], (D, CONV_CH), D ** -0.5, 0.125, ((0, 32), (1, 2))),
        "w_conv_value": scatter_about(streams_of[4], (D, CONV_CH), D ** -0.5, 0.125, ((0, 32), (1, 2))),
        "conv_taps": scatter_about(streams_of[5], (3, CONV_CH), 3 ** -0.5, 3.5, ((1, 2),), jnp.float32),
        "w_receptance": scatter_about(streams_of[6], (D, STATE_CH), D ** -0.5, 0.125, ((0, 32), (1, 2))),
        "w_key": scatter_about(streams_of[7], (D, STATE_CH), D ** -0.5, 0.125, ((0, 32), (1, 2))),
        "w_value": scatter_about(streams_of[8], (D, STATE_CH), D ** -0.5, 0.125, ((0, 32), (1, 2))),
        "w_decay_down": scatter_about(streams_of[9], (D, DECAY_RANK), D ** -0.5, 0.125, ((0, 32),)),
        "w_decay_up": scatter_about(streams_of[10], (DECAY_RANK, STATE_CH), (DECAY_RANK // 2) ** -0.5, 0.75, ((1, 2),)),
        "decay_base": draw_decay_base(jax.random.fold_in(streams_of[21], 71), 0),
        "decay_shift": draw_decay_shift(jax.random.fold_in(streams_of[21], 71), 0),
        "w_rate_down": scatter_about(streams_of[13], (D, RATE_RANK), D ** -0.5, 0.125, ((0, 32),)),
        "w_rate_up": scatter_about(streams_of[14], (RATE_RANK, STATE_CH), RATE_RANK ** -0.5, 0.5, ((1, 2),)),
        "rate_base": draw_rate_base(jax.random.fold_in(streams_of[21], 71), 0),
        "key_scale": jnp.clip(jnp.exp(math.log(2.5) - 2.3025851 * jax.random.uniform(streams_of[16], (STATE_CH,), jnp.float32) ** level_of(streams_of[16], (STATE_CH,), ((0, 2),), -0.2, 0.2)), 0.25, 2.5),
        "key_mix": jnp.clip(0.1 + 0.59999999 * jax.random.uniform(streams_of[17], (STATE_CH,), jnp.float32) ** level_of(streams_of[17], (STATE_CH,), ((0, 2),), -0.2, 0.2), 0.1, 0.7),
        "group_gain": jnp.clip(1.0 + 0.18 * jax.random.normal(streams_of[18], (STATE_CH,), jnp.float32), 0.1, 1.9),
        "w_out_conv": scatter_about(streams_of[19], (CONV_CH, D), (CONV_CH + STATE_CH) ** -0.5, 0.125, ((0, 2), (1, 32))),
        "w_out_state": scatter_about(streams_of[20], (STATE_CH, D), (CONV_CH + STATE_CH) ** -0.5, 0.125, ((0, 2), (1, 32))),
    }


highest = lax.Precision.HIGHEST

def normalize_rows(rows_in, norm_gain):
    values = rows_in.astype(jnp.float32)
    scaled = values * lax.rsqrt(lax.optimization_barrier(jnp.mean(values * values, axis=-1, keepdims=True)) + 1e-06)
    return (scaled * norm_gain).astype(jnp.bfloat16)

def project(normed, weight):
    return jnp.dot(normed, weight, preferred_element_type=jnp.float32).astype(jnp.bfloat16)

def recurrence(receptance, decay_mul, key_write, value_vec, erase_vec, replace_vec):

    def advance(memory, inputs_now):
        recv_now, decay_now, key_now, value_now, erase_now, replace_now = inputs_now
        erased = jnp.einsum('hvk,hk->hv', memory, erase_now, precision=highest)
        memory = memory * decay_now[:, None, :] + erased[:, :, None] * replace_now[:, None, :] + value_now[:, :, None] * key_now[:, None, :]
        return (memory, jnp.einsum('hvk,hk->hv', memory, recv_now, precision=highest))
    initial = jnp.zeros((HEADS, HEAD, HEAD), jnp.float32)
    return lax.scan(advance, initial, (receptance, decay_mul, key_write, value_vec, erase_vec, replace_vec))[1]

def merge_outputs(conv_out, state_out, w_out_conv, w_out_state):
    filter_branch_output = CONV_CH // N_TP
    state_part = STATE_CH // N_TP
    combined = jnp.zeros((conv_out.shape[0], w_out_conv.shape[1]), jnp.float32)
    for member in range(N_TP):
        conv_lo = member * filter_branch_output
        state_lo = member * state_part
        partial_sum = jnp.dot(conv_out[:, conv_lo:conv_lo + filter_branch_output], w_out_conv[conv_lo:conv_lo + filter_branch_output], preferred_element_type=jnp.float32) + jnp.dot(state_out[:, state_lo:state_lo + state_part], w_out_state[state_lo:state_lo + state_part], preferred_element_type=jnp.float32)
        rounded = lax.optimization_barrier(partial_sum.astype(jnp.bfloat16))
        combined = combined + rounded.astype(jnp.float32)
    return combined.astype(jnp.bfloat16)

def split_heads(values):
    return values.reshape(values.shape[0], HEADS, HEAD)

def reference(tokens, norm_gain, w_conv_gate, w_conv_in, w_conv_value, conv_taps, w_receptance, w_key, w_value, w_decay_down, w_decay_up, decay_base, decay_shift, w_rate_down, w_rate_up, rate_base, key_scale, key_mix, group_gain, w_out_conv, w_out_state):
    results = []
    for sequence in range(BATCH_SERIES):
        normed = normalize_rows(tokens[sequence], norm_gain)
        conv_gate = project(normed, w_conv_gate)
        filter_source = project(normed, w_conv_in)
        conv_value = project(normed, w_conv_value)
        product_value = filter_source.astype(jnp.float32) * conv_value.astype(jnp.float32)
        padded = jnp.concatenate([jnp.zeros((2, CONV_CH), jnp.float32), product_value], axis=0)
        filtered = conv_taps[0] * padded[:-2] + conv_taps[1] * padded[1:-1] + conv_taps[2] * padded[2:]
        conv_out = (conv_gate.astype(jnp.float32) * filtered).astype(jnp.bfloat16)
        receptance = project(normed, w_receptance)
        key_raw = project(normed, w_key)
        value_raw = project(normed, w_value)
        decay_low = project(normed, w_decay_down)
        rate_low = project(normed, w_rate_down)
        decay_act = jnp.tanh(decay_low.astype(jnp.float32)).astype(jnp.bfloat16)
        decay_pre = decay_base + jnp.dot(decay_act, w_decay_up, preferred_element_type=jnp.float32)
        log_decay = decay_shift[sequence] - jnp.exp(-jax.nn.softplus(-decay_pre) - 0.5)
        learn_rate = jax.nn.sigmoid(rate_base + jnp.dot(rate_low, w_rate_up, preferred_element_type=jnp.float32))
        scaled_key = split_heads(key_raw.astype(jnp.float32) * key_scale)
        erase_dir = scaled_key * lax.rsqrt(lax.optimization_barrier(jnp.sum(scaled_key * scaled_key, axis=-1, keepdims=True)) + 1e-06)
        key_write = key_raw.astype(jnp.float32) * (1.0 + (learn_rate - 1.0) * key_mix)
        readouts = recurrence(split_heads(receptance.astype(jnp.float32)), split_heads(jnp.exp(log_decay)), split_heads(key_write), split_heads(value_raw.astype(jnp.float32)), -erase_dir, erase_dir * split_heads(learn_rate))
        centered = readouts - lax.optimization_barrier(jnp.mean(readouts, axis=-1, keepdims=True))
        variance = lax.optimization_barrier(jnp.mean(centered * centered, axis=-1, keepdims=True))
        normal_heads = (centered * lax.rsqrt(variance + 0.00064)).reshape(SERIES_STEPS, STATE_CH)
        state_out = (normal_heads * group_gain).astype(jnp.bfloat16)
        results.append(merge_outputs(conv_out, state_out, w_out_conv, w_out_state))
    return jnp.stack(results)
```

```python
import jax
import jax.numpy as jnp
from jax import lax
from jax.experimental import pallas as pl
from jax.experimental.pallas import tpu as pltpu
from jax.sharding import Mesh
from jax.sharding import PartitionSpec as P

SP = ("sp_0", "sp_1")
SP_TP = ("sp_0", "sp_1", "tp")

f32, bf16 = jnp.float32, jnp.bfloat16
HEAD = 64
LANES = 128
STEPS = 256
BLOCK = 32
HALF = 128
SLOTS = 4
norm_eps = 1e-06
group_eps = 0.00064
highest = lax.Precision.HIGHEST


def mm(a, b, form="nn"):
    dims = {"nn": ((1,), (0,)), "nt": ((1,), (1,)), "tn": ((0,), (0,))}[form]
    return lax.dot_general(
        a.astype(bf16), b.astype(bf16), (dims, ((), ())), preferred_element_type=f32
    )


def mm_exact(a, b):
    return lax.dot_general(
        a, b, (((1,), (0,)), ((), ())), precision=highest, preferred_element_type=f32
    )


def iota2(shape, dim):
    return lax.broadcasted_iota(jnp.int32, shape, dim)


def at_row(values, row):
    blocks = values.reshape(STEPS // BLOCK, BLOCK, LANES)
    return jnp.broadcast_to(blocks[:, row : row + 1, :], blocks.shape).reshape(values.shape)


def unit_terms(rec, key, low_d, low_r, shift, up_d, up_r, par):
    base_d, base_r, scale, mix = (par[k : k + 1] for k in range(4))
    act = jnp.tanh(low_d.astype(f32)).astype(bf16)
    pre = base_d + mm(act, up_d)
    log_decay = shift - jax.nn.sigmoid(pre) * 0.6065306597126334
    rate = jax.nn.sigmoid(base_r + mm(low_r, up_r))
    key = key.astype(f32)
    rec = rec.astype(f32)
    same_head = ((iota2((LANES, LANES), 0) < HEAD) == (iota2((LANES, LANES), 1) < HEAD))
    scaled = key * scale
    length = mm_exact(scaled * scaled, same_head.astype(f32))
    erase = scaled * lax.rsqrt(length + norm_eps)
    write = key * (1.0 + (rate - 1.0) * mix)
    rows, cols = iota2((STEPS, STEPS), 0), iota2((STEPS, STEPS), 1)
    running = ((rows >= cols) & (rows // BLOCK == cols // BLOCK)).astype(f32)
    total = mm_exact(running, log_decay)
    middle = at_row(total, BLOCK // 2 - 1)
    final = at_row(total, BLOCK - 1)
    up = jnp.exp(total - middle)
    down = jnp.exp(middle - total)
    to_start = jnp.exp(middle)
    erase_mid = -erase * jnp.exp(total - log_decay - middle)
    query_mid = rec * up
    replace = erase * rate
    replace_mid = replace * down
    write_mid = write * down
    tail = jnp.exp(final - total)
    return (
        erase_mid,
        query_mid,
        replace_mid,
        write_mid,
        erase_mid * to_start,
        query_mid * to_start,
        replace * tail,
        write * tail,
        jnp.exp(final),
    )


def chunk_kernel(units, *refs):
    reads, (shift_ref, upd_ref, upr_ref, par_ref, query_ref, local_ref, send_ref) = (
        refs[1:11], refs[11:18])
    lane = iota2((HALF, LANES), 1)
    t_row, s_col = iota2((HALF, HALF), 0), iota2((HALF, HALF), 1)
    same = t_row // BLOCK == s_col // BLOCK
    strict = same & (t_row > s_col)
    causal = same & (t_row >= s_col)
    head_lane = (lane < HEAD, lane >= HEAD)
    terms, chains = [], []
    for u in range(units):
        rec, key, val, low_d, low_r = (
            jnp.concatenate([reads[2 * k][0, u], reads[2 * k + 1][0, u]], axis=0) for k in range(5)
        )
        val = val.astype(f32)
        got = unit_terms(
            rec, key, low_d, low_r, shift_ref[u], upd_ref[...], upr_ref[...], par_ref[...]
        )
        terms.append(got + (val, pltpu.roll(val, HEAD, 1)))
    for u in range(units):
        (erase_mid, query_mid, replace_mid, write_mid, erase_0, query_0, replace_end,
         write_end, whole, val, val_turned) = terms[u]
        for half in range(2):
            cut = slice(half * HALF, (half + 1) * HALF)
            right = jnp.concatenate([replace_mid[cut], write_mid[cut]], axis=0)
            left = jnp.concatenate([erase_mid[cut], query_mid[cut]], axis=0)
            for head in range(2):
                mine = head_lane[head]
                both = jnp.concatenate([mine, mine], axis=0)
                pairs = mm(jnp.where(both, left, 0.0), right, "nt")
                erase_replace = jnp.where(strict, pairs[:HALF, :HALF], 0.0).astype(bf16)
                erase_key = jnp.where(strict, pairs[:HALF, HALF:], 0.0)
                query_both = jnp.concatenate(
                    [jnp.where(causal, pairs[HALF:, :HALF], 0.0),
                     jnp.where(causal, pairs[HALF:, HALF:], 0.0)], axis=1).astype(bf16)
                val_mine = jnp.where(mine, 0.0, val_turned[cut]).astype(bf16)
                first = jnp.where(mine, erase_0[cut], 0.0) + mm(erase_key, val_mine)
                chains.append([erase_replace, first, query_both, val_mine])
    for stage in range(5):
        for chain in chains:
            power, solved = chain[0], chain[1]
            if stage < 4:
                made = mm(power, jnp.concatenate([power, solved.astype(bf16)], axis=1))
                chain[0] = made[:, :HALF].astype(bf16)
                chain[1] = solved + made[:, HALF:]
            else:
                chain[1] = solved + mm(power, solved)
    sq = iota2((LANES, LANES), 0) < HEAD
    sl = iota2((LANES, LANES), 1) < HEAD
    same_head = sq == sl
    states, maps, adds, wholes, queries, locals_ = [], [], [], [], [], []
    for u in range(units):
        (erase_mid, query_mid, replace_mid, write_mid, erase_0, query_0, replace_end,
         write_end, whole, val, val_turned) = terms[u]
        start, local_erase, query, local = [], [], [], []
        for half in range(2):
            cut = slice(half * HALF, (half + 1) * HALF)
            one, two = chains[u * 4 + half * 2], chains[u * 4 + half * 2 + 1]
            low = head_lane[0]
            start.append(jnp.where(low, one[1], two[1]))
            local_erase.append(pltpu.roll(jnp.where(low, two[1], one[1]), HEAD, 1))
            outs = [
                mm(c[2], jnp.concatenate([c[1].astype(bf16), c[3]], axis=0)) for c in (one, two)
            ]
            query.append(query_0[cut] + jnp.where(low, outs[0], outs[1]))
            local.append(pltpu.roll(jnp.where(low, outs[1], outs[0]), HEAD, 1))
        start = jnp.concatenate(start, axis=0).astype(bf16)
        local_erase = jnp.concatenate(local_erase, axis=0).astype(bf16)
        queries.append(jnp.concatenate(query, axis=0).astype(bf16))
        locals_.append(jnp.concatenate(local, axis=0))
        replace_end, write_end, vb = (a.astype(bf16) for a in (replace_end, write_end, val))
        unit_maps, unit_adds, unit_whole = [], [], []
        for n in range(STEPS // BLOCK):
            cut = slice(n * BLOCK, (n + 1) * BLOCK)
            moved = mm(start[cut], replace_end[cut], "tn")
            unit_maps.append(jnp.where(same_head, moved, 0.0).astype(bf16))
            put = mm(
                jnp.concatenate([local_erase[cut], vb[cut]], axis=0),
                jnp.concatenate([replace_end[cut], write_end[cut]], axis=0), "tn")
            unit_adds.append(jnp.where(sl[:HEAD], put[:HEAD], put[HEAD:]))
            unit_whole.append(whole[n * BLOCK : n * BLOCK + 1])
        maps.append(unit_maps)
        adds.append(unit_adds)
        wholes.append(unit_whole)
        eye = (iota2((HEAD, LANES), 0) == iota2((HEAD, LANES), 1) % HEAD).astype(f32)
        states.append(jnp.concatenate([eye, jnp.zeros((HEAD, LANES), f32)], axis=0))
    for n in range(STEPS // BLOCK):
        for u in range(units):
            state = states[u]
            lo = sl[:HEAD]
            top, bottom = state[:HEAD], state[HEAD:]
            wide = jnp.concatenate(
                [jnp.where(lo, top, 0.0), jnp.where(lo, 0.0, top),
                 jnp.where(lo, bottom, 0.0), jnp.where(lo, 0.0, bottom)], axis=0)
            cut = slice(n * BLOCK, (n + 1) * BLOCK)
            seen = mm(queries[u][cut], wide, "nt")
            query_ref[u, cut, :] = seen[:, :LANES].astype(bf16)
            local_ref[u, cut, :] = locals_[u][cut] + seen[:, LANES:]
            moved = state * wholes[u][n] + mm(state, maps[u][n])
            states[u] = jnp.concatenate([moved[:HEAD], moved[HEAD:] + adds[u][n]], axis=0)
    low = head_lane[0]
    for u in range(units):
        both = (states[u], pltpu.roll(states[u], HEAD, 1))
        for head in range(2):
            mine, other = both[head], both[1 - head]
            packed = jnp.where(low[:BLOCK], mine[:BLOCK], other[BLOCK:HEAD]).astype(bf16)
            for piece in range(4):
                place = (2 * u + head) * 4 + piece
                row = HEAD + 16 * piece
                send_ref[place, :BLOCK, :] = packed
                send_ref[place, BLOCK:, :] = jnp.where(
                    low[:8], mine[row : row + 8], other[row + 8 : row + 16]).astype(bf16)


def chunk_terms(core, projected, shift, up_d, up_r, par, units=2, first_col=3):
    part = lambda k, half: pl.BlockSpec(
        (1, units, HALF, LANES), lambda i, c: (c[0] ^ half, i, 0, first_col + k))
    full = lambda shape: pl.BlockSpec(shape, lambda i, c: tuple(0 for _ in shape))
    rows = lambda shape: pl.BlockSpec(shape, lambda i, c: (i, 0, 0))
    return pl.pallas_call(
        lambda *refs: chunk_kernel(units, *refs),
        grid_spec=pltpu.PrefetchScalarGridSpec(
            num_scalar_prefetch=1,
            grid=(SLOTS // units,),
            in_specs=[part(k, half) for k in range(5) for half in range(2)] + [
                rows((units, STEPS, LANES)), full((LANES, LANES)), full((LANES, LANES)),
                full((8, LANES)),
            ],
            out_specs=[
                rows((units, STEPS, LANES)), rows((units, STEPS, LANES)),
                rows((8 * units, BLOCK + 8, LANES)),
            ],
        ),
        out_shape=[
            jax.ShapeDtypeStruct((SLOTS, STEPS, LANES), bf16),
            jax.ShapeDtypeStruct((SLOTS, STEPS, LANES), f32),
            jax.ShapeDtypeStruct((8 * SLOTS, BLOCK + 8, LANES), bf16),
        ],
        cost_estimate=pl.CostEstimate(
            flops=8 * 10**9, bytes_accessed=4 * 10**6, transcendentals=10**6),
        name="chunk_terms",
    )(core, *[projected] * 10, shift, up_d, up_r, par)


def chain_kernel(got_ref, out_ref):
    low = iota2((BLOCK, LANES), 1) < HEAD
    devices = got_ref.shape[0]
    zeros = jnp.zeros((HEAD, LANES), bf16)
    state = jnp.zeros((16, LANES), f32)
    for i in range(devices):
        turned = pltpu.roll(state, HEAD, 1)
        out_ref[i] = jnp.where(low[:8], state[:8], turned[8:]).astype(bf16)
        if i == devices - 1:
            break
        packed = got_ref[i].astype(f32)
        packed_turned = pltpu.roll(packed, HEAD, 1)
        step = jnp.concatenate(
            [jnp.where(low, packed[:BLOCK], 0.0).astype(bf16),
             jnp.where(low, packed_turned[:BLOCK], 0.0).astype(bf16), zeros], axis=0)
        add = jnp.concatenate(
            [jnp.where(low[:8], packed[BLOCK:], 0.0),
             jnp.where(low[:8], packed_turned[BLOCK:], 0.0)], axis=0)
        top = state.astype(bf16)
        rest = (state - top.astype(f32)).astype(bf16)
        moved = mm(jnp.concatenate([top, rest], axis=0), step)
        state = moved[:16] + moved[16:] + add


def chain_states(got):
    return pl.pallas_call(
        chain_kernel,
        out_shape=jax.ShapeDtypeStruct((got.shape[0], 8, LANES), bf16),
        cost_estimate=pl.CostEstimate(flops=10**9, bytes_accessed=10**6, transcendentals=0),
        name="chain_states",
    )(got)


def finish_kernel(core, gate0, gate1, in0, in1, value0, value1, halo_ref, query_ref, local_ref,
                  enter_ref, w_ref, par_ref, out_ref):
    row = iota2((STEPS, LANES), 0)
    low8 = iota2((8, LANES), 1) < HEAD
    whole = lambda a, b: jnp.concatenate([a[0, 0], b[0, 0]], axis=0).astype(f32)
    gate, source, value = whole(gate0, gate1), whole(in0, in1), whole(value0, value1)
    product = source * value
    halo = halo_ref[0].astype(f32)
    before = halo[:2] * halo[2:]
    one = jnp.where(row == 0, before[1:2], pltpu.roll(product, 1, 0))
    two = jnp.where(row == 0, before[:1], jnp.where(row == 1, before[1:2], pltpu.roll(product, 2, 0)))
    par = par_ref[...]
    filtered = par[4:5] * two + par[5:6] * one + par[6:7] * product
    conv_out = (gate * filtered).astype(bf16)
    blocks = []
    for head in range(2):
        for piece in range(4):
            got = enter_ref[head * 4 + piece].astype(f32)
            turned = pltpu.roll(got, HEAD, 1)
            pair = (got, turned) if head == 0 else (turned, got)
            keep = low8 if head == 0 else ~low8
            blocks += [jnp.where(keep, half, 0.0) for half in pair]
    entering = jnp.concatenate(blocks, axis=0)
    readout = local_ref[0] + mm(query_ref[0], entering, "nt")
    same_head = (iota2((LANES, LANES), 0) < HEAD) == (iota2((LANES, LANES), 1) < HEAD)
    average = jnp.where(same_head, 1.0 / HEAD, 0.0)
    centered = readout - mm_exact(readout, average)
    variance = mm_exact(centered * centered, average)
    state_out = (centered * lax.rsqrt(variance + group_eps) * par[7:8]).astype(bf16)
    both = jnp.concatenate([conv_out, state_out], axis=1)
    partial = mm(both, w_ref[...], "nt").astype(bf16)
    mine = core[0]
    out_ref[mine, 0] = partial[:HALF]
    out_ref[1 - mine, 0] = partial[HALF:]


def finish(core, projected, halo, query, local, enter, w_out, par):
    width = w_out.shape[0]
    part = lambda k, half: pl.BlockSpec(
        (1, 1, HALF, LANES), lambda i, c: (c[0] ^ half, i, 0, k))
    full = lambda shape: pl.BlockSpec(shape, lambda i, c: tuple(0 for _ in shape))
    rows = lambda shape: pl.BlockSpec(shape, lambda i, c: (i, 0, 0))
    return pl.pallas_call(
        finish_kernel,
        grid_spec=pltpu.PrefetchScalarGridSpec(
            num_scalar_prefetch=1,
            grid=(SLOTS,),
            in_specs=[part(k, half) for k in range(3) for half in range(2)] + [
                rows((1, 4, LANES)), rows((1, STEPS, LANES)), rows((1, STEPS, LANES)),
                rows((8, 8, LANES)), full((width, 2 * LANES)), full((8, LANES)),
            ],
            out_specs=pl.BlockSpec((2, 1, HALF, width), lambda i, c: (0, i, 0, 0)),
        ),
        out_shape=jax.ShapeDtypeStruct((2, SLOTS, HALF, width), bf16),
        cost_estimate=pl.CostEstimate(
            flops=2 * 10**9, bytes_accessed=8 * 10**6, transcendentals=10**5),
        name="finish",
    )(core, *[projected] * 6, halo, query, local, enter, w_out, par)


def to_offset(block, axis, distance):
    devices = lax.axis_size(axis)
    return lax.ppermute(block, axis, [(i, (i + distance) % devices) for i in range(devices)])


def from_behind(block, axis):
    devices = lax.axis_size(axis)
    return lax.ppermute(block, axis, [(i - 1, i) for i in range(1, devices)])


def exchange(shard, axis):
    return lax.all_to_all(shard, axis, 0, 0, tiled=True)


def mine_of(array, axis, dim):
    return lax.dynamic_slice_in_dim(array, lax.axis_index(axis) * LANES, LANES, dim)


def normalize_rows(norm_gain, row_piece):
    values = row_piece.astype(f32)
    scaled = values * lax.rsqrt(jnp.mean(values * values, axis=-1, keepdims=True) + norm_eps)
    return (scaled * norm_gain).astype(bf16)


def gather_slots(block, axis):
    middle = block.shape[0] // 2
    behind = to_offset(block, axis, 1)
    ahead = to_offset(block, axis, -1)
    opposite = (to_offset(behind[:middle], axis, 1), to_offset(ahead[middle:], axis, -1))
    return [block, behind, ahead, *opposite]


def scatter_slots(shift, axis):
    here = lax.axis_index(axis)
    piece = lambda d: lax.dynamic_slice_in_dim(shift, ((here + d) % SLOTS) * LANES, LANES, 1)
    return jnp.stack(
        [piece(0)] + [to_offset(piece(d), axis, d) for d in (1, -1, 2)])


def sum_slots(parts, axis):
    own, behind, ahead, opposite = (parts[k] for k in range(SLOTS))
    middle = own.shape[0] // 2
    add = lambda a, b: (a.astype(f32) + b.astype(f32)).astype(bf16)
    first = to_offset(opposite[:middle], axis, 1)
    second = to_offset(opposite[middle:], axis, -1)
    ahead = jnp.concatenate([add(ahead[:middle], first), ahead[middle:]], axis=0)
    behind = jnp.concatenate([behind[:middle], add(behind[middle:], second)], axis=0)
    from_left, from_right = to_offset(ahead, axis, 1), to_offset(behind, axis, -1)
    return own.astype(f32) + from_left.astype(f32) + from_right.astype(f32)


def body(
    tokens, norm_gain, w_conv_gate, w_conv_in, w_conv_value, conv_taps, w_receptance, w_key,
    w_value, w_decay_down, w_decay_up, decay_base, decay_shift, w_rate_down, w_rate_up, rate_base,
    key_scale, key_mix, group_gain, w_out_conv, w_out_state,
):
    core = lax.axis_index("tp").astype(jnp.int32)[None]
    mine = lambda a, dim: mine_of(a, "fs", dim)
    normed = normalize_rows(norm_gain, tokens[0])
    own = gather_slots(normed, "fs")
    other = [to_offset(block, "tp", 1) for block in own]
    rows = jnp.concatenate(own + other, axis=0)
    columns = [
        mine(w, 1) for w in (w_conv_gate, w_conv_in, w_conv_value, w_receptance, w_key, w_value)
    ]
    w_in = lax.all_gather(
        jnp.concatenate(columns + [w_decay_down, w_rate_down], axis=1), SP, axis=0, tiled=True)
    w_out = lax.all_gather(
        jnp.concatenate([mine(w_out_conv, 0), mine(w_out_state, 0)], axis=0).T,
        SP, axis=0, tiled=True)
    shift = scatter_slots(decay_shift[0], "fs")
    par = jnp.concatenate(
        [mine(a, 0)[None] for a in (decay_base, rate_base, key_scale, key_mix)]
        + [mine(conv_taps, 1), mine(group_gain, 0)[None]], axis=0)
    projected = jnp.dot(rows, w_in, preferred_element_type=f32).astype(bf16)
    projected = projected.reshape(2, SLOTS, HALF, w_in.shape[1])
    last = lax.dynamic_index_in_dim(projected, 1 - core[0], 0, keepdims=False)[:, -2:]
    halo = jnp.concatenate([last[:, :, LANES : 2 * LANES], last[:, :, 2 * LANES : 3 * LANES]], axis=1)
    halo = from_behind(halo, SP)
    query, local, send = chunk_terms(
        core, projected, shift, mine(w_decay_up, 1), mine(w_rate_up, 1), par)
    enter = exchange(chain_states(exchange(send, SP)), SP)
    partial = finish(core, projected, halo, query, local, enter, w_out, par)
    shared = (
        partial[0].astype(f32) + to_offset(partial[1], "tp", 1).astype(f32)
    ).astype(bf16)
    return sum_slots(shared, "fs").astype(bf16)[None]


def solution(mesh):
    split = Mesh(
        mesh.devices.reshape(8, 4, mesh.shape["fs"], mesh.shape["tp"]), ("sp_0", "sp_1", "fs", "tp")
    )
    placed = (
        P("fs", SP_TP, None),
        P(),
        P(SP, "tp"),
        P(SP, "tp"),
        P(SP, "tp"),
        P(None, "tp"),
        P(SP, "tp"),
        P(SP, "tp"),
        P(SP, "tp"),
        P(SP, None),
        P(None, "tp"),
        P("tp"),
        P("fs", SP, "tp"),
        P(SP, None),
        P(None, "tp"),
        P("tp"),
        P("tp"),
        P("tp"),
        P("tp"),
        P("tp", SP),
        P("tp", SP),
    )
    return jax.shard_map(
        body, mesh=split, in_specs=placed, out_specs=P("fs", SP_TP, None), check_vma=False
    )
```

```python
import jax
import jax.numpy as jnp
from jax import lax
from jax.experimental import pallas as pl
from jax.experimental.pallas import tpu as pltpu
from jax.sharding import Mesh
from jax.sharding import PartitionSpec as P

SP = ("sp_0", "sp_1")
SP_TP = ("sp_0", "sp_1", "tp")

f32, bf16 = jnp.float32, jnp.bfloat16
HEAD = 64
LANES = 128
STEPS = 256
BLOCK = 32
HALF = 128
SLOTS = 4
RING_Y = (0, -1, 1, 2)
WIDE = 4 * HEAD
STATE_COLS = 5 * LANES
CONV_COLS = 3 * LANES
norm_eps = 1e-06
group_eps = 0.00064
highest = lax.Precision.HIGHEST


def mm(a, b, form="nn"):
    dims = {"nn": ((1,), (0,)), "nt": ((1,), (1,)), "tn": ((0,), (0,))}[form]
    return lax.dot_general(
        a.astype(bf16), b.astype(bf16), (dims, ((), ())), preferred_element_type=f32
    )


def mm_exact(a, b):
    return lax.dot_general(
        a, b, (((1,), (0,)), ((), ())), precision=highest, preferred_element_type=f32
    )


def mm_two(a, b):
    top = a.astype(bf16)
    rest = (a - top.astype(f32)).astype(bf16)
    made = mm(jnp.concatenate([top, rest], axis=0), b)
    return made[: a.shape[0]] + made[a.shape[0] :]


def iota2(shape, dim):
    return lax.broadcasted_iota(jnp.int32, shape, dim)


def at_row(values, row):
    blocks = values.reshape(STEPS // BLOCK, BLOCK, LANES)
    return jnp.broadcast_to(blocks[:, row : row + 1, :], blocks.shape).reshape(values.shape)


def unit_terms(rec, key, low_d, low_r, shift, up_d, up_r, par):
    base_d, base_r, scale, mix = (par[k : k + 1] for k in range(4))
    act = jnp.tanh(low_d.astype(f32)).astype(bf16)
    pre = base_d + mm(act, up_d)
    log_decay = shift - jax.nn.sigmoid(pre) * 0.6065306597126334
    rate = jax.nn.sigmoid(base_r + mm(low_r, up_r))
    key = key.astype(f32)
    rec = rec.astype(f32)
    same_head = ((iota2((LANES, LANES), 0) < HEAD) == (iota2((LANES, LANES), 1) < HEAD))
    scaled = key * scale
    length = mm_two(scaled * scaled, same_head.astype(f32))
    erase = scaled * lax.rsqrt(length + norm_eps)
    write = key * (1.0 + (rate - 1.0) * mix)
    rows, cols = iota2((STEPS, STEPS), 0), iota2((STEPS, STEPS), 1)
    running = ((rows >= cols) & (rows // BLOCK == cols // BLOCK)).astype(f32)
    total = mm_exact(running, log_decay)
    middle = at_row(total, BLOCK // 2 - 1)
    final = at_row(total, BLOCK - 1)
    up = jnp.exp(total - middle)
    down = jnp.exp(middle - total)
    to_start = jnp.exp(middle)
    erase_mid = -erase * jnp.exp(total - log_decay - middle)
    query_mid = rec * up
    replace = erase * rate
    replace_mid = replace * down
    write_mid = write * down
    tail = jnp.exp(final - total)
    return (
        erase_mid,
        query_mid,
        replace_mid,
        write_mid,
        erase_mid * to_start,
        query_mid * to_start,
        replace * tail,
        write * tail,
        jnp.exp(final),
    )


def chunk_kernel(units, *refs):
    reads, (upd_ref, upr_ref, par_ref, query_ref, local_ref, send_ref) = (
        refs[1:11], refs[15:21])
    shifts = refs[11:15]
    first_step = pl.program_id(0) == 0
    lane = iota2((HALF, LANES), 1)
    t_row, s_col = iota2((HALF, HALF), 0), iota2((HALF, HALF), 1)
    same = t_row // BLOCK == s_col // BLOCK
    strict = same & (t_row > s_col)
    causal = same & (t_row >= s_col)
    head_lane = (lane < HEAD, lane >= HEAD)
    terms, chains = [], []
    for u in range(units):
        rec, key, val, low_d, low_r = (
            jnp.concatenate([reads[2 * k][0, u], reads[2 * k + 1][0, u]], axis=0) for k in range(5)
        )
        val = val.astype(f32)
        shift = jnp.where(first_step, shifts[u][...], shifts[units + u][...])
        got = unit_terms(
            rec, key, low_d, low_r, shift, upd_ref[...], upr_ref[...], par_ref[...]
        )
        terms.append(got + (val, pltpu.roll(val, HEAD, 1)))
    for u in range(units):
        (erase_mid, query_mid, replace_mid, write_mid, erase_0, query_0, replace_end,
         write_end, whole, val, val_turned) = terms[u]
        for half in range(2):
            cut = slice(half * HALF, (half + 1) * HALF)
            right = jnp.concatenate([replace_mid[cut], write_mid[cut]], axis=0)
            left = jnp.concatenate([erase_mid[cut], query_mid[cut]], axis=0)
            for head in range(2):
                mine = head_lane[head]
                both = jnp.concatenate([mine, mine], axis=0)
                pairs = mm(jnp.where(both, left, 0.0), right, "nt")
                erase_replace = jnp.where(strict, pairs[:HALF, :HALF], 0.0).astype(bf16)
                erase_key = jnp.where(strict, pairs[:HALF, HALF:], 0.0)
                query_both = jnp.concatenate(
                    [jnp.where(causal, pairs[HALF:, :HALF], 0.0),
                     jnp.where(causal, pairs[HALF:, HALF:], 0.0)], axis=1).astype(bf16)
                val_mine = jnp.where(mine, 0.0, val_turned[cut]).astype(bf16)
                first = jnp.where(mine, erase_0[cut], 0.0) + mm(erase_key, val_mine)
                chains.append([erase_replace, first, query_both, val_mine])
    for stage in range(5):
        for chain in chains:
            power, solved = chain[0], chain[1]
            if stage < 4:
                made = mm(power, jnp.concatenate([power, solved.astype(bf16)], axis=1))
                chain[0] = made[:, :HALF].astype(bf16)
                chain[1] = solved + made[:, HALF:]
            else:
                chain[1] = solved + mm(power, solved)
    sq = iota2((LANES, LANES), 0) < HEAD
    sl = iota2((LANES, LANES), 1) < HEAD
    same_head = sq == sl
    states, maps, adds, wholes, queries, locals_ = [], [], [], [], [], []
    for u in range(units):
        (erase_mid, query_mid, replace_mid, write_mid, erase_0, query_0, replace_end,
         write_end, whole, val, val_turned) = terms[u]
        start, local_erase, query, local = [], [], [], []
        for half in range(2):
            cut = slice(half * HALF, (half + 1) * HALF)
            one, two = chains[u * 4 + half * 2], chains[u * 4 + half * 2 + 1]
            low = head_lane[0]
            start.append(jnp.where(low, one[1], two[1]))
            local_erase.append(pltpu.roll(jnp.where(low, two[1], one[1]), HEAD, 1))
            outs = [
                mm(c[2], jnp.concatenate([c[1].astype(bf16), c[3]], axis=0)) for c in (one, two)
            ]
            query.append(query_0[cut] + jnp.where(low, outs[0], outs[1]))
            local.append(pltpu.roll(jnp.where(low, outs[1], outs[0]), HEAD, 1))
        start = jnp.concatenate(start, axis=0).astype(bf16)
        local_erase = jnp.concatenate(local_erase, axis=0).astype(bf16)
        queries.append(jnp.concatenate(query, axis=0).astype(bf16))
        locals_.append(jnp.concatenate(local, axis=0))
        replace_end, write_end, vb = (a.astype(bf16) for a in (replace_end, write_end, val))
        unit_maps, unit_adds, unit_whole = [], [], []
        for n in range(STEPS // BLOCK):
            cut = slice(n * BLOCK, (n + 1) * BLOCK)
            moved = mm(start[cut], replace_end[cut], "tn")
            unit_maps.append(jnp.where(same_head, moved, 0.0).astype(bf16))
            put = mm(
                jnp.concatenate([local_erase[cut], vb[cut]], axis=0),
                jnp.concatenate([replace_end[cut], write_end[cut]], axis=0), "tn")
            unit_adds.append(jnp.where(sl[:HEAD], put[:HEAD], put[HEAD:]))
            unit_whole.append(whole[n * BLOCK : n * BLOCK + 1])
        maps.append(unit_maps)
        adds.append(unit_adds)
        wholes.append(unit_whole)
        eye = (iota2((HEAD, LANES), 0) == iota2((HEAD, LANES), 1) % HEAD).astype(f32)
        states.append(jnp.concatenate([eye, jnp.zeros((HEAD, LANES), f32)], axis=0))
    for n in range(STEPS // BLOCK):
        for u in range(units):
            state = states[u]
            lo = sl[:HEAD]
            top, bottom = state[:HEAD], state[HEAD:]
            wide = jnp.concatenate(
                [jnp.where(lo, top, 0.0), jnp.where(lo, 0.0, top),
                 jnp.where(lo, bottom, 0.0), jnp.where(lo, 0.0, bottom)], axis=0)
            cut = slice(n * BLOCK, (n + 1) * BLOCK)
            seen = mm(queries[u][cut], wide, "nt")
            query_ref[u, cut, :] = seen[:, :LANES].astype(bf16)
            local_ref[u, cut, :] = locals_[u][cut] + seen[:, LANES:]
            moved = state * wholes[u][n] + mm(state, maps[u][n])
            states[u] = jnp.concatenate([moved[:HEAD], moved[HEAD:] + adds[u][n]], axis=0)
    low = head_lane[0]
    for u in range(units):
        both = (states[u], pltpu.roll(states[u], HEAD, 1))
        for head in range(2):
            mine, other = both[head], both[1 - head]
            packed = jnp.where(low[:BLOCK], mine[:BLOCK], other[BLOCK:HEAD]).astype(bf16)
            for piece in range(4):
                place = (2 * u + head) * 4 + piece
                row = HEAD + 16 * piece
                send_ref[place, :BLOCK, :] = packed
                send_ref[place, BLOCK:, :] = jnp.where(
                    low[:8], mine[row : row + 8], other[row + 8 : row + 16]).astype(bf16)


def chunk_terms(here, projected, shift, up_d, up_r, par, units=2):
    part = lambda k, half: pl.BlockSpec(
        (1, units, HALF, LANES), lambda i, c: (c[0] ^ half, i, 0, k))
    mine = pl.BlockSpec((LANES, LANES), lambda i, c: (0, c[1]))
    full = lambda shape: pl.BlockSpec(shape, lambda i, c: tuple(0 for _ in shape))
    rows = lambda shape: pl.BlockSpec(shape, lambda i, c: (i, 0, 0))
    return pl.pallas_call(
        lambda *refs: chunk_kernel(units, *refs),
        grid_spec=pltpu.PrefetchScalarGridSpec(
            num_scalar_prefetch=1,
            grid=(SLOTS // units,),
            in_specs=[part(k, half) for k in range(5) for half in range(2)] + [
                full((STEPS, LANES))] + [full((STEPS, LANES))] * (SLOTS - 1) + [mine, mine, full((8, LANES)),
            ],
            out_specs=[
                rows((units, STEPS, LANES)), rows((units, STEPS, LANES)),
                rows((8 * units, BLOCK + 8, LANES)),
            ],
        ),
        out_shape=[
            jax.ShapeDtypeStruct((SLOTS, STEPS, LANES), bf16),
            jax.ShapeDtypeStruct((SLOTS, STEPS, LANES), f32),
            jax.ShapeDtypeStruct((8 * SLOTS, BLOCK + 8, LANES), bf16),
        ],
        cost_estimate=pl.CostEstimate(
            flops=8 * 10**9, bytes_accessed=4 * 10**6, transcendentals=10**6),
        name="chunk_terms",
    )(here, *[projected] * 10, *shift, up_d, up_r, par)


def chain_kernel(got_ref, out_ref):
    low = iota2((BLOCK, LANES), 1) < HEAD
    devices = got_ref.shape[0]
    zeros = jnp.zeros((HEAD, LANES), bf16)
    state = jnp.zeros((16, LANES), f32)
    for i in range(devices):
        turned = pltpu.roll(state, HEAD, 1)
        out_ref[i] = jnp.where(low[:8], state[:8], turned[8:]).astype(bf16)
        if i == devices - 1:
            break
        packed = got_ref[i].astype(f32)
        packed_turned = pltpu.roll(packed, HEAD, 1)
        step = jnp.concatenate(
            [jnp.where(low, packed[:BLOCK], 0.0).astype(bf16),
             jnp.where(low, packed_turned[:BLOCK], 0.0).astype(bf16), zeros], axis=0)
        add = jnp.concatenate(
            [jnp.where(low[:8], packed[BLOCK:], 0.0),
             jnp.where(low[:8], packed_turned[BLOCK:], 0.0)], axis=0)
        top = state.astype(bf16)
        rest = (state - top.astype(f32)).astype(bf16)
        moved = mm(jnp.concatenate([top, rest], axis=0), step)
        state = moved[:16] + moved[16:] + add


def chain_states(got):
    return pl.pallas_call(
        chain_kernel,
        out_shape=jax.ShapeDtypeStruct((got.shape[0], 8, LANES), bf16),
        cost_estimate=pl.CostEstimate(flops=10**9, bytes_accessed=10**6, transcendentals=0),
        name="chain_states",
    )(got)


def store_halves(core, values, own_ref, other_ref, slot):
    for c in range(2):

        @pl.when(core[0] == c)
        def _(c=c):
            own_ref[slot] = values[c * HALF : (c + 1) * HALF]
            other_ref[slot] = values[(1 - c) * HALF : (2 - c) * HALF]


def conv_kernel(core, *refs):
    parts, (halo_ref, par_ref, own_ref, other_ref) = refs[:6], refs[6:]
    row = iota2((STEPS, LANES), 0)
    par = par_ref[...]
    for u in range(SLOTS):
        gate, source, value = (
            jnp.concatenate([parts[2 * k][0, u], parts[2 * k + 1][0, u]], axis=0).astype(f32)
            for k in range(3)
        )
        product = source * value
        halo = halo_ref[u].astype(f32)
        before = halo[:2] * halo[2:]
        one = jnp.where(row == 0, before[1:2], pltpu.roll(product, 1, 0))
        two = jnp.where(
            row == 0, before[:1], jnp.where(row == 1, before[1:2], pltpu.roll(product, 2, 0)))
        filtered = par[4:5] * two + par[5:6] * one + par[6:7] * product
        store_halves(core, (gate * filtered).astype(bf16), own_ref, other_ref, u)


def half_outputs():
    whole = (SLOTS, HALF, LANES)
    return dict(
        out_specs=[pl.BlockSpec(whole, lambda i, c: (0, 0, 0))] * 2,
    ), [jax.ShapeDtypeStruct(whole, bf16)] * 2


def convolve(here, rows, halo, par):
    part = lambda k, half: pl.BlockSpec(
        (1, SLOTS, HALF, LANES), lambda i, c: (c[0] ^ half, 0, 0, k))
    full = lambda shape: pl.BlockSpec(shape, lambda i, c: tuple(0 for _ in shape))
    specs, shapes = half_outputs()
    return pl.pallas_call(
        conv_kernel,
        grid_spec=pltpu.PrefetchScalarGridSpec(
            num_scalar_prefetch=1, grid=(1,),
            in_specs=[part(k, half) for k in range(3) for half in range(2)]
            + [full(halo.shape), full(par.shape)], **specs),
        out_shape=shapes,
        cost_estimate=pl.CostEstimate(flops=10**7, bytes_accessed=2 * 10**6, transcendentals=0),
        name="convolve",
    )(here, *[rows] * 6, halo, par)


def readout_kernel(core, query_ref, local_ref, enter_ref, par_ref, own_ref, other_ref):
    low8 = iota2((8, LANES), 1) < HEAD
    same_head = (iota2((LANES, LANES), 0) < HEAD) == (iota2((LANES, LANES), 1) < HEAD)
    average = jnp.where(same_head, 1.0 / HEAD, 0.0)
    for u in range(SLOTS):
        blocks = []
        for head in range(2):
            for piece in range(4):
                got = enter_ref[u * 8 + head * 4 + piece].astype(f32)
                turned = pltpu.roll(got, HEAD, 1)
                pair = (got, turned) if head == 0 else (turned, got)
                keep = low8 if head == 0 else ~low8
                blocks += [jnp.where(keep, half, 0.0) for half in pair]
        entering = jnp.concatenate(blocks, axis=0)
        readout = local_ref[u] + mm(query_ref[u], entering, "nt")
        centered = readout - mm_two(readout, average)
        variance = mm_two(centered * centered, average)
        state_out = centered * lax.rsqrt(variance + group_eps) * par_ref[7:8, :]
        store_halves(core, state_out.astype(bf16), own_ref, other_ref, u)


def read_states(here, query, local, enter, par):
    full = lambda a: pl.BlockSpec(a.shape, lambda i, c: tuple(0 for _ in a.shape))
    specs, shapes = half_outputs()
    return pl.pallas_call(
        readout_kernel,
        grid_spec=pltpu.PrefetchScalarGridSpec(
            num_scalar_prefetch=1, grid=(1,),
            in_specs=[full(a) for a in (query, local, enter, par)], **specs),
        out_shape=shapes,
        cost_estimate=pl.CostEstimate(flops=10**9, bytes_accessed=2 * 10**6, transcendentals=10**4),
        name="read_states",
    )(here, query, local, enter, par)


def product_kernel(conv_own, state_own, conv_peer, state_peer, w_own, w_peer, out_ref):
    own = jnp.concatenate([conv_own[0], state_own[0]], axis=1)
    peer = jnp.concatenate([conv_peer[0], state_peer[0]], axis=1)
    out_ref[0] = (mm(own, w_own[...], "nt") + mm(peer, w_peer[...], "nt")).astype(bf16)


def product(conv_own, state_own, conv_peer, state_peer, w_own, w_peer):
    width = w_own.shape[0]
    rows = pl.BlockSpec((1, HALF, LANES), lambda i: (i, 0, 0))
    full = pl.BlockSpec(w_own.shape, lambda i: (0, 0))
    return pl.pallas_call(
        product_kernel,
        grid=(SLOTS,),
        in_specs=[rows] * 4 + [full] * 2,
        out_specs=pl.BlockSpec((1, HALF, width), lambda i: (i, 0, 0)),
        out_shape=jax.ShapeDtypeStruct((SLOTS, HALF, width), bf16),
        cost_estimate=pl.CostEstimate(
            flops=2 * 10**9, bytes_accessed=4 * 10**6, transcendentals=0),
        name="product",
    )(conv_own, state_own, conv_peer, state_peer, w_own, w_peer)


def pack_kernel(here, *refs):
    (gate, source, value, rec, key, val, down_d, down_r, out_conv, out_state, a_ref, b_ref) = refs
    state = jnp.concatenate([r[...] for r in (rec, key, val, down_d, down_r)], axis=1)
    conv = jnp.concatenate([r[...] for r in (out_conv, out_state, gate, source, value)], axis=1)
    for k in range(a_ref.shape[0]):
        a_ref[k] = state
        b_ref[k] = conv


def pack(here, copies, *weights):
    shard = weights[0].shape[0]
    mine = pl.BlockSpec((shard, LANES), lambda i, c: (0, c[1]))
    whole = pl.BlockSpec((shard, LANES), lambda i, c: (0, 0))
    packed = jax.ShapeDtypeStruct((copies, shard, STATE_COLS), bf16)
    full = pl.BlockSpec((copies, shard, STATE_COLS), lambda i, c: (0, 0, 0))
    return pl.pallas_call(
        pack_kernel,
        grid_spec=pltpu.PrefetchScalarGridSpec(
            num_scalar_prefetch=1, grid=(1,),
            in_specs=[mine] * 6 + [whole] * 2 + [mine] * 2, out_specs=[full, full]),
        out_shape=[packed, packed],
        cost_estimate=pl.CostEstimate(flops=10**7, bytes_accessed=10**6, transcendentals=0),
        name="pack",
    )(here, *weights)


def join_kernel(*refs):
    at = 0
    for ref in refs[:-1]:
        refs[-1][at : at + ref.shape[0]] = ref[...]
        at += ref.shape[0]


def join(pieces):
    rows = sum(piece.shape[0] for piece in pieces)
    return pl.pallas_call(
        join_kernel,
        out_shape=jax.ShapeDtypeStruct((rows, *pieces[0].shape[1:]), bf16),
        cost_estimate=pl.CostEstimate(flops=10**7, bytes_accessed=10**6, transcendentals=0),
    )(*pieces)


def place_rows(here, pieces, span, target):
    own, behind, ahead, *opposite = pieces
    depth = own.shape[0] // HEAD
    for z in range(depth):
        each = depth // len(opposite)
        for y, (ref, row) in enumerate(
            ((own, z), (behind, z), (ahead, z), (opposite[z // each], z % each))
        ):
            start = z * WIDE + lax.rem(here[3] + (RING_Y[y] + 4), 4) * HEAD
            target[pl.ds(pl.multiple_of(start, HEAD), HEAD), :] = ref[
                row * HEAD : (row + 1) * HEAD, span]


def project_rows(own_ref, other_ref, weights, out_ref):
    for k, ref in enumerate((own_ref, other_ref)):

        @pl.loop(0, SLOTS // 2)
        def _(i, k=k, ref=ref):
            span = pl.ds(pl.multiple_of(i * 2 * HALF, 2 * HALF), 2 * HALF)
            made = jnp.dot(ref[span, :], weights[...], preferred_element_type=f32).astype(bf16)
            out_ref[k, i * 2] = made[:HALF]
            out_ref[k, i * 2 + 1] = made[HALF:]


def project_state_kernel(here, own_ref, other_ref, *refs):
    w_refs, (out_ref, weights) = refs[:-2], refs[-2:]
    place_rows(here, w_refs, slice(None), weights)
    project_rows(own_ref, other_ref, weights, out_ref)


def project_conv_kernel(here, own_ref, other_ref, *refs):
    w_refs, (out_ref, w_out_ref, weights) = refs[:-3], refs[-3:]
    place_rows(here, w_refs, slice(0, 2 * LANES), w_out_ref)
    place_rows(here, w_refs, slice(2 * LANES, STATE_COLS), weights)
    project_rows(own_ref, other_ref, weights, out_ref)


def project(kernel, here, own, other, weights, cols, extra):
    width = own.shape[1]
    full = lambda shape: pl.BlockSpec(shape, lambda i, c: tuple(0 for _ in shape))
    shapes = [jax.ShapeDtypeStruct((2, SLOTS, HALF, cols), bf16)]
    shapes += [jax.ShapeDtypeStruct((width, extra), bf16)] if extra else []
    ins = (own, other, *weights)
    return pl.pallas_call(
        kernel,
        grid_spec=pltpu.PrefetchScalarGridSpec(
            num_scalar_prefetch=1, grid=(1,),
            in_specs=[full(a.shape) for a in ins], out_specs=[full(a.shape) for a in shapes],
            scratch_shapes=[pltpu.VMEM((width, cols), bf16)]),
        out_shape=shapes,
        compiler_params=pltpu.CompilerParams(vmem_limit_bytes=40 * 2**20),
        cost_estimate=pl.CostEstimate(
            flops=2 * 1024 * width * cols, bytes_accessed=8 * 10**6, transcendentals=0),
    )(here, *ins)


def to_offset(block, axis, distance):
    devices = lax.axis_size(axis)
    return lax.ppermute(block, axis, [(i, (i + distance) % devices) for i in range(devices)])


def from_behind(block, axis):
    devices = lax.axis_size(axis)
    return lax.ppermute(block, axis, [(i - 1, i) for i in range(1, devices)])


def exchange(shard, axis):
    return lax.all_to_all(shard, axis, 0, 0, tiled=True)


def mine_of(array, axis, dim):
    return lax.dynamic_slice_in_dim(array, lax.axis_index(axis) * LANES, LANES, dim)


def normalize_rows(norm_gain, row_piece):
    values = row_piece.astype(f32)
    scaled = values * lax.rsqrt(jnp.mean(values * values, axis=-1, keepdims=True) + norm_eps)
    return (scaled * norm_gain).astype(bf16)


def gather_slots(block, axis, halves):
    middle = block.shape[0] // 2
    behind = to_offset(block, axis, 1)
    ahead = to_offset(block, axis, -1)
    if halves:
        opposite = [to_offset(behind[:middle], axis, 1), to_offset(ahead[middle:], axis, -1)]
    else:
        opposite = [to_offset(behind, axis, 1)]
    return [block, behind, ahead, *opposite]


def scatter_slots(shift, axis):
    here = lax.axis_index(axis)
    piece = lambda d: lax.dynamic_slice_in_dim(shift, ((here + d) % SLOTS) * LANES, LANES, 1)
    return [piece(0)] + [
        to_offset(piece(d), axis, d) for d in (1, -1, 2)]


def sum_slots(parts, axis):
    own, behind, ahead, opposite = (parts[k] for k in range(SLOTS))
    middle = own.shape[0] // 2
    add = lambda a, b: (a.astype(f32) + b.astype(f32)).astype(bf16)
    first = to_offset(opposite[:middle], axis, 1)
    second = to_offset(opposite[middle:], axis, -1)
    ahead = jnp.concatenate([add(ahead[:middle], first), ahead[middle:]], axis=0)
    behind = jnp.concatenate([behind[:middle], add(behind[middle:], second)], axis=0)
    from_left = to_offset(ahead, axis, 1)
    from_right = to_offset(behind, axis, -1)
    return own.astype(f32) + from_left.astype(f32) + from_right.astype(f32)


def body(
    tokens, norm_gain, w_conv_gate, w_conv_in, w_conv_value, conv_taps, w_receptance, w_key,
    w_value, w_decay_down, w_decay_up, decay_base, decay_shift, w_rate_down, w_rate_up, rate_base,
    key_scale, key_mix, group_gain, w_out_conv, w_out_state,
):
    here = jnp.stack([lax.axis_index(a) for a in ("tp", "fs", "sp_0", "sp_1")]).astype(jnp.int32)
    mine = lambda a, dim: mine_of(a, "fs", dim)
    state_w, conv_w = pack(
        here, lax.axis_size("sp_0"), w_conv_gate, w_conv_in, w_conv_value, w_receptance, w_key,
        w_value, w_decay_down, w_rate_down, w_out_conv.T, w_out_state.T)
    flat = lambda w: w.reshape(-1, w.shape[2])
    normed = normalize_rows(norm_gain, tokens[0])
    own = join(gather_slots(normed, "fs", False))
    other = to_offset(own, "tp", 1)
    state_w = gather_slots(flat(exchange(state_w, "sp_0")), "sp_1", True)
    conv_w = gather_slots(flat(exchange(conv_w, "sp_0")), "sp_1", True)
    shift = scatter_slots(decay_shift[0], "fs")
    par = jnp.concatenate(
        [mine(a, 0)[None] for a in (decay_base, rate_base, key_scale, key_mix)]
        + [mine(conv_taps, 1), mine(group_gain, 0)[None]], axis=0)
    (state_rows,) = project(
        project_state_kernel, here, own, other, state_w, STATE_COLS, 0)
    query, local, send = chunk_terms(here, state_rows, shift, w_decay_up, w_rate_up, par)
    conv_rows, w_own = project(
        project_conv_kernel, here, own, other, conv_w, CONV_COLS, 2 * LANES)
    w_peer = to_offset(w_own, "tp", 1)
    last = lax.dynamic_index_in_dim(conv_rows, 1 - here[0], 0, keepdims=False)[:, -2:]
    halo = jnp.concatenate([last[:, :, LANES : 2 * LANES], last[:, :, 2 * LANES :]], axis=1)
    halo = from_behind(halo, SP)
    conv_own, conv_other = convolve(here, conv_rows, halo, par)
    conv_peer = to_offset(conv_other, "tp", 1)
    states = chain_states(exchange(send, SP))
    enter = exchange(states, SP)
    state_own, state_other = read_states(here, query, local, enter, par)
    state_peer = to_offset(state_other, "tp", 1)
    shared = product(conv_own, state_own, conv_peer, state_peer, w_own, w_peer)
    return sum_slots(shared, "fs").astype(bf16)[None]


def solution(mesh):
    split = Mesh(
        mesh.devices.reshape(8, 4, mesh.shape["fs"], mesh.shape["tp"]), ("sp_0", "sp_1", "fs", "tp")
    )
    placed = (
        P("fs", SP_TP, None),
        P(),
        P(SP, "tp"),
        P(SP, "tp"),
        P(SP, "tp"),
        P(None, "tp"),
        P(SP, "tp"),
        P(SP, "tp"),
        P(SP, "tp"),
        P(SP, None),
        P(None, "tp"),
        P("tp"),
        P("fs", SP, "tp"),
        P(SP, None),
        P(None, "tp"),
        P("tp"),
        P("tp"),
        P("tp"),
        P("tp"),
        P("tp", SP),
        P("tp", SP),
    )
    return jax.shard_map(
        body, mesh=split, in_specs=placed, out_specs=P("fs", SP_TP, None), check_vma=False
    )
```
